512 devices in a mesh: fs: 32 (over z, core), tp: 16 (over y, x).
Axes of the slice: x: 4, y: 4, z: 16, core: 2. Of those that a mesh axis runs over, the one named last changes fastest.
Arguments:
- normed_in: bfloat16 [32768, 2048], P('fs'), may hold values from -6 to 6
- grad_x: bfloat16 [32768, 2048], P('fs', 'tp'), may hold values from -0.044194174 to 0.044194174
- grad_y: bfloat16 [32768, 2048], P('fs', 'tp'), may hold values from -0.044194174 to 0.044194174
- weight_x: float32 [2048, 2048], P('fs', 'tp'), may hold values from -0.125 to 0.125
- weight_y: float32 [2048, 2048], P('fs', 'tp'), may hold values from -0.125 to 0.125
- factor_x: bfloat16 [2048, 512], P('fs'), may hold values from -0.13258252 to 0.13258252
- factor_y: bfloat16 [2048, 512], P('fs'), may hold values from -0.13258252 to 0.13258252
- first_x: float32 [512, 2048], P('fs', 'tp'), may hold values from -8 to 8
- first_y: float32 [512, 2048], P('fs', 'tp'), may hold values from -8 to 8
- second_x: float32 [512, 2048], P('fs', 'tp'), may hold values from 0.5 to 2
- second_y: float32 [512, 2048], P('fs', 'tp'), may hold values from 0.5 to 2
Outputs:
- new_weight_x: float32 [2048, 2048], P('fs', 'tp')
- new_weight_y: float32 [2048, 2048], P('fs', 'tp')
- step_x: float32 [2048, 2048], P('fs', 'tp')
- step_y: float32 [2048, 2048], P('fs', 'tp')
- new_first_x: float32 [512, 2048], P('fs', 'tp')
- new_first_y: float32 [512, 2048], P('fs', 'tp')
- new_second_x: float32 [512, 2048], P('fs', 'tp')
- new_second_y: float32 [512, 2048], P('fs', 'tp')
- copy_x: bfloat16 [2048, 2048], P(None, 'tp')
- copy_y: bfloat16 [2048, 2048], P(None, 'tp')
The draws below stay inside these ranges and needn't reach their ends.
All inputs are finite; a program needn't handle non-finite values.
Results may differ from the reference program's by a relative error of at most 0.02.
Values may be sent and summed in bfloat16 or wider, within the bound.
A program may use at most 128 MiB of HBM per device.

```python
import math
import jax
import jax.numpy as jnp
from jax import lax

D = 2048
RW = 2048
RANK = 512
TOKENS = 32768


def noise_block(key, shape):
    return jnp.clip(jax.random.normal(key, shape, jnp.float32), -6.0, 6.0)


def bounded_normal(key, shape):
    return jnp.clip(jax.random.normal(key, shape, jnp.float32), -3.0, 3.0)


def token_scales(key):
    return bounded_normal(jax.random.fold_in(key, 101), (TOKENS,))


def draw_normed_in(key, part):
    feature = bounded_normal(jax.random.fold_in(key, 102), (D,))
    background = noise_block(jax.random.fold_in(key, 103), (TOKENS, D))
    mixed = background + 0.5 * token_scales(key)[:, None] * feature[None, :]
    return jnp.clip(mixed, -6.0, 6.0).astype(jnp.bfloat16)


def cotangent_draw(key, tag):
    strength = 12.0
    channel = bounded_normal(jax.random.fold_in(key, tag), (RW,))
    background = noise_block(jax.random.fold_in(key, tag + 1), (TOKENS, RW)) * TOKENS ** (-0.5)
    coherent = strength / TOKENS * token_scales(key)[:, None] * channel[None, :]
    ceiling = 8.0 * TOKENS ** (-0.5)
    return jnp.clip(background + coherent, -ceiling, ceiling).astype(jnp.bfloat16)


def draw_grad_x(key, part):
    return cotangent_draw(key, 201)


def draw_grad_y(key, part):
    return cotangent_draw(key, 211)


def factor_draw(key, tag):
    shared_weight = 0.1
    common = bounded_normal(jax.random.fold_in(key, tag), (D,))
    spread_block = noise_block(jax.random.fold_in(key, tag + 1), (D, RANK))
    ceiling = 6.0 * D ** (-0.5)
    factor = (spread_block + shared_weight * common[:, None]) * D ** (-0.5)
    return jnp.clip(factor, -ceiling, ceiling).astype(jnp.bfloat16)


def draw_factor_x(key, part):
    return factor_draw(key, 301)


def draw_factor_y(key, part):
    return factor_draw(key, 311)


def moment_draw(key, tag):
    column_mean = bounded_normal(jax.random.fold_in(key, tag), (RW,))
    ripple = noise_block(jax.random.fold_in(key, tag + 1), (RANK, RW))
    return jnp.clip(ripple + column_mean[None, :], -8.0, 8.0)


def draw_first_x(key, part):
    return moment_draw(key, 401)


def draw_first_y(key, part):
    return moment_draw(key, 411)


def level_of(rng, shape, split, least, top_value):
    level, own = 1.0, jax.random.fold_in(rng, 6)
    for position, parts in split:
        draws = jnp.exp(jax.random.uniform(jax.random.fold_in(own, position), (parts,), jnp.float32, least / len(split), top_value / len(split)))
        level = level * jnp.repeat(draws, shape[position] // parts).reshape([-1 if axis == position else 1 for axis in range(len(shape))])
    return level


def gaussian(stream_key, shape, deviation, bound, split=(), dtype=jnp.bfloat16):
    array = deviation * jax.random.normal(stream_key, shape, jnp.float32)
    if split:
        array = array * level_of(stream_key, shape, split, -0.22, 0.18)
    return jnp.clip(array, -bound, bound).astype(dtype)


def setup_inputs(seed: int = 0) -> dict:
    key_of = jax.random.split(jax.random.key(seed), 12)
    normed_in = draw_normed_in(jax.random.fold_in(key_of[11], 71), 0)
    grad_x = draw_grad_x(jax.random.fold_in(key_of[11], 71), 0)
    grad_y = draw_grad_y(jax.random.fold_in(key_of[11], 71), 0)
    weight_x = gaussian(key_of[3], (D, RW), D ** -0.5, 0.125, ((0, 32), (1, 16)), jnp.float32)
    weight_y = gaussian(key_of[4], (D, RW), D ** -0.5, 0.125, ((0, 32), (1, 16)), jnp.float32)
    factor_x = draw_factor_x(jax.random.fold_in(key_of[11], 71), 0)
    factor_y = draw_factor_y(jax.random.fold_in(key_of[11], 71), 0)
    first_x = draw_first_x(jax.random.fold_in(key_of[11], 71), 0)
    first_y = draw_first_y(jax.random.fold_in(key_of[11], 71), 0)
    second_x = jnp.clip(jnp.exp(math.log(2.0) - 1.3862944 * jax.random.uniform(key_of[9], (RANK, RW), jnp.float32) ** level_of(key_of[9], (RANK, RW), ((0, 32), (1, 16)), -0.2, 0.2)), 0.5, 2.0)
    second_y = jnp.clip(jnp.exp(math.log(2.0) - 1.3862944 * jax.random.uniform(key_of[10], (RANK, RW), jnp.float32) ** level_of(key_of[10], (RANK, RW), ((0, 32), (1, 16)), -0.2, 0.2)), 0.5, 2.0)
    return {"normed_in": normed_in, "grad_x": grad_x, "grad_y": grad_y, "weight_x": weight_x, "weight_y": weight_y, "factor_x": factor_x, "factor_y": factor_y, "first_x": first_x, "first_y": first_y, "second_x": second_x, "second_y": second_y}


def branch(normed_in, cotangent, factor, first, second):
    gradient = lax.dot_general(normed_in, cotangent, (((0,), (0,)), ((), ())), preferred_element_type=jnp.float32)
    factor_full = factor.astype(jnp.float32)
    low = jnp.dot(factor_full.T, gradient, precision=lax.Precision.HIGHEST)
    first_new = 0.8 * first + 0.2 * low
    second_new = 0.9 * second + 0.1 * low * low
    direction = first_new / jnp.sqrt(second_new)
    update = jnp.dot(factor_full, direction, precision=lax.Precision.HIGHEST)
    return (update, first_new, second_new)

def reference(normed_in, grad_x, grad_y, weight_x, weight_y, factor_x, factor_y, first_x, first_y, second_x, second_y):
    update_x, first_new_x, second_new_x = branch(normed_in, grad_x, factor_x, first_x, second_x)
    update_y, first_new_y, second_new_y = branch(normed_in, grad_y, factor_y, first_y, second_y)
    total = jnp.sum(update_x * update_x) + jnp.sum(update_y * update_y)
    scale = jnp.minimum(1.0, 0.25 * jnp.sqrt(2.0 * D * RW) / jnp.sqrt(total))
    step_x = scale * update_x
    step_y = scale * update_y
    new_x = weight_x - 0.02 * step_x
    new_y = weight_y - 0.02 * step_y
    return (new_x, new_y, step_x, step_y, first_new_x, first_new_y, second_new_x, second_new_y, new_x.astype(jnp.bfloat16), new_y.astype(jnp.bfloat16))
```

```python
import functools

import jax
import jax.numpy as jnp
from jax import lax
from jax.experimental import pallas as pl
from jax.experimental.pallas import tpu as pltpu
from jax.sharding import Mesh
from jax.sharding import PartitionSpec as P

D = 2048
RW = 2048
NZ = 16
FS = ("z", "c")
TP = ("y", "x")
MESH_ID = pl.DeviceIdType.MESH
F32 = jnp.float32
BF16 = jnp.bfloat16


def wait_on(ref, sem):
    pltpu.make_async_copy(ref, ref, sem).wait()


def body(
    n_hbm, gx_hbm, gy_hbm, wx_hbm, wy_hbm, fx_hbm, fy_hbm, ax_hbm, ay_hbm, sx_hbm, sy_hbm,
    nwx, nwy, stx, sty, nfx, nfy, nsx, nsy, cpx, cpy,
    n_v, g_v, f_loc, w_loc, m_loc, f_all, g_f, g_in, g_hl, lo_out, lo_in, d_out, d_all,
    u_f, u_b, u_ob, u_of, w_all, w_tmp, w_oth, s_out, s_all,
    ld, za_s, z_r, zb_s, ip_s, ip_r, pr_s, pr_r, wr_s, wr_r, far_s, lo_r, d_r, s_r,
):
    z, c, y, x = (lax.axis_index(k) for k in ("z", "c", "y", "x"))
    zz = lambda k: lax.rem(z + (k + NZ), NZ)
    other = 1 - c
    partner = (z, other, y, x)

    def send(src, dst, ssem, rsem, dev):
        pltpu.make_async_remote_copy(
            src_ref=src, dst_ref=dst, send_sem=ssem, recv_sem=rsem, device_id=dev, device_id_type=MESH_ID
        ).start()

    barrier = pltpu.get_barrier_semaphore()
    place = c * 16 + y * 4 + x

    def at_place(q):
        return (z, q // 16, lax.rem(q // 4, 4), lax.rem(q, 4))

    @pl.loop(1, 5)
    def _(k):
        for cc in range(2):
            for sign in (1, -1):
                pl.semaphore_signal(
                    barrier, inc=1, device_id=(lax.rem(z + sign * k + NZ, NZ), cc, y, x), device_id_type=MESH_ID
                )

    @pl.loop(1, 32)
    def _(k):
        pl.semaphore_signal(barrier, inc=1, device_id=at_place(lax.rem(place + k, 32)), device_id_type=MESH_ID)

    f_in = [pltpu.make_async_copy(r, f_loc.at[i], ld.at[i]) for i, r in enumerate((fx_hbm, fy_hbm))]
    w_in = [pltpu.make_async_copy(r, w_loc.at[i], ld.at[2 + i]) for i, r in enumerate((wx_hbm, wy_hbm))]
    g_ld = [
        pltpu.make_async_copy(r, g_v.at[:, pl.ds(128 * i, 128)], ld.at[4 + i]) for i, r in enumerate((gx_hbm, gy_hbm))
    ]
    m_in = [
        pltpu.make_async_copy(r, m_loc.at[i], ld.at[6 + i]) for i, r in enumerate((ax_hbm, ay_hbm, sx_hbm, sy_hbm))
    ]
    for cp in f_in + w_in + g_ld:
        cp.start()

    @pl.loop(0, NZ)
    def _(i):
        col = pl.multiple_of(128 * lax.rem(z + i + (NZ - 4), NZ), 128)
        pltpu.make_async_copy(
            n_hbm.at[:, pl.ds(col, 128)], n_v.at[:, pl.ds(pl.multiple_of(128 * i, 128), 128)], ld.at[10]
        ).start()

    for cp in m_in:
        cp.start()
    for cp in f_in + w_in:
        cp.wait()

    f_all[4, pl.ds(pl.multiple_of(64 * c, 64), 64), :] = f_loc[c]
    w_all[4, pl.ds(pl.multiple_of(64 * c, 64), 64), :] = w_loc[c].astype(BF16)
    w_tmp[...] = w_loc[other].astype(BF16)
    pl.semaphore_wait(barrier, 47)

    for br, (a, b) in enumerate(((y, x), (x, y))):
        rg, ch = 2 * a + b // 2, lax.rem(b, 2)
        cols = pl.ds(pl.multiple_of(256 * ch, 256), 256)

        @pl.when(c == a // 2)
        def _():
            for n, k in enumerate((4, -4, 3, -3, 2, -2, 1, -1)):
                send(
                    f_loc.at[br, pl.ds(pl.multiple_of(16 * lax.rem(rg, 4), 16), 16), cols],
                    f_all.at[4 - k, pl.ds(pl.multiple_of(16 * rg, 16), 16), cols],
                    za_s.at[br, n],
                    z_r.at[4 - k],
                    (zz(k), br, y, x),
                )

    mine = pl.ds(pl.multiple_of(64 * c, 64), 64)
    theirs = pl.ds(pl.multiple_of(64 * other, 64), 64)
    send(w_tmp, w_all.at[4, mine, :], pr_s.at[0], pr_r.at[0], partner)
    send(f_loc.at[other], f_all.at[4, mine, :], pr_s.at[1], pr_r.at[1], partner)

    right = (zz(1), c, y, x)
    left = (zz(-1), c, y, x)

    def ring(s):
        if s > 1:
            wait_on(w_all.at[(5 - s) % NZ], wr_r.at[0, s - 2])
        send(w_all.at[(5 - s) % NZ], w_all.at[(4 - s) % NZ], wr_s.at[0, s - 1], wr_r.at[0, s - 1], right)
        if s < 8:
            if s > 1:
                wait_on(w_all.at[3 + s], wr_r.at[1, s - 2])
            send(w_all.at[3 + s], w_all.at[4 + s], wr_s.at[1, s - 1], wr_r.at[1, s - 1], left)

    wait_on(w_all.at[4, theirs, :], pr_r.at[0])
    ring(1)

    for cp in g_ld:
        cp.wait()
    wait_on(n_v, ld.at[10])
    for t in range(4):
        cols = slice(512 * t, 512 * t + 512)
        r = lax.dot_general(g_v[...], n_v[:, cols], (((0,), (0,)), ((), ())), preferred_element_type=F32)
        g_f[0, :, cols] = r[:128]
        g_f[1, :, cols] = r[128:]
    send(g_f.at[other], g_in, pr_s.at[2], pr_r.at[2], partner)

    ra = jnp.where(c == 0, y, x)
    rb = jnp.where(c == 0, x, y)

    def part1(lo, n, b):
        rg, ch = 2 * ra + b // 2, lax.rem(b, 2)
        return f_all.at[
            pl.ds(lo, n), pl.ds(pl.multiple_of(16 * rg, 16), 16), pl.ds(pl.multiple_of(256 * ch, 256), 256)
        ]

    def part2(lo, n, a):
        return f_all.at[pl.ds(lo, n), pl.ds(pl.multiple_of(32 * a, 32), 32), :]

    def dev1(k):
        b = lax.rem(rb + k + 4, 4)
        return b, (z, c, jnp.where(c == 0, y, b), jnp.where(c == 0, b, x))

    def dev2(k):
        a = lax.rem(ra + k + 4, 4)
        return a, (z, c, jnp.where(c == 0, a, y), jnp.where(c == 0, x, a))

    groups = ((0, 4), (5, 4), (9, 7))

    def plane_first(g, ph):
        lo, n = groups[g]
        part, dev, me = ((part1, dev1, rb), (part2, dev2, ra))[ph]
        for i, k in enumerate((1, -1)):
            send(part(lo, n, me), part(lo, n, me), ip_s.at[g, ph, i], ip_r.at[g, ph, i], dev(k)[1])

    def plane_second(g, ph):
        lo, n = groups[g]
        h = (n + 1) // 2
        part, dev = ((part1, dev1), (part2, dev2))[ph]
        lft, rgt = dev(-1), dev(1)
        wait_on(part(lo, n, lft[0]), ip_r.at[g, ph, 0])
        send(part(lo, h, lft[0]), part(lo, h, lft[0]), ip_s.at[g, ph, 2], ip_r.at[g, ph, 2], rgt[1])
        wait_on(part(lo, n, rgt[0]), ip_r.at[g, ph, 1])
        send(
            part(lo + h, n - h, rgt[0]), part(lo + h, n - h, rgt[0]), ip_s.at[g, ph, 3], ip_r.at[g, ph, 3], lft[1]
        )

    def plane_third(g, ph):
        lo, n = groups[g]
        h = (n + 1) // 2
        part, dev = ((part1, dev1), (part2, dev2))[ph]
        far = dev(2)[0]
        wait_on(part(lo, h, far), ip_r.at[g, ph, 2])
        wait_on(part(lo + h, n - h, far), ip_r.at[g, ph, 3])

    def slab(i):
        return part1(i, 1, rb)

    wait_on(slab(0), z_r.at[0])
    for m in (4, 3, 2, 1):
        send(slab(0), slab(NZ - m), zb_s.at[0, m - 1], z_r.at[NZ - m], (zz(m), c, y, x))
    wait_on(slab(8), z_r.at[8])
    for m in (3, 2, 1):
        send(slab(8), slab(8 + m), zb_s.at[1, m - 1], z_r.at[8 + m], (zz(-m), c, y, x))
    for i in (1, 2, 3):
        wait_on(slab(i), z_r.at[i])
    plane_first(0, 0)
    for i in (5, 6, 7):
        wait_on(slab(i), z_r.at[i])
    plane_first(1, 0)
    ring(2)
    wait_on(g_in, pr_r.at[2])
    for t in range(4):
        cols = slice(512 * t, 512 * t + 512)
        g = g_f[c, :, cols] + g_in[:, cols]
        hi = g.astype(BF16)
        g_hl[:128, cols] = hi
        g_hl[128:, cols] = (g - hi.astype(F32)).astype(BF16)

    plane_second(0, 0)
    plane_second(1, 0)
    ring(3)
    plane_third(0, 0)
    plane_first(0, 1)
    plane_third(1, 0)
    plane_first(1, 1)
    for i in range(9, 16):
        wait_on(slab(i), z_r.at[i])
    plane_first(2, 0)
    ring(4)
    plane_second(2, 0)
    plane_second(0, 1)
    plane_second(1, 1)
    plane_third(2, 0)
    plane_first(2, 1)
    ring(5)
    plane_third(0, 1)
    plane_third(1, 1)
    wait_on(f_all.at[4, theirs, :], pr_r.at[1])

    def low_of(lo, n):
        return jnp.dot(
            g_hl[:, 128 * lo : 128 * (lo + n)],
            f_all[lo : lo + n].reshape(128 * n, 512),
            preferred_element_type=F32,
        )

    low = low_of(0, 9)
    plane_second(2, 1)
    plane_third(2, 1)
    low = low + low_of(9, 7)
    low = (low[:128] + low[128:]).T
    lo_out[...] = low.astype(BF16).reshape(32, 16, 128)

    @pl.loop(0, NZ)
    def _(i):
        k = lax.rem(i, 2) * (8 + (i + 1) // 2) + (1 - lax.rem(i, 2)) * (8 - i // 2)
        zt = lax.rem(z + k, NZ)
        for ct in range(2):
            @pl.when((k > 0) & (k < NZ))
            def _():
                send(
                    lo_out.at[2 * zt + ct], lo_in.at[c, z], far_s.at[zt, ct], lo_r.at[c, z], (zt, ct, y, x)
                )

    lo_in[c, z] = lo_out[2 * z + c]
    send(lo_out.at[2 * z + other], lo_in.at[c, z], far_s.at[z, other], lo_r.at[c, z], partner)
    ring(6)
    for cp in m_in:
        cp.wait()

    @pl.loop(0, NZ)
    def _(i):
        for b in range(2):
            @pl.when((i != z) | (b != c))
            def _():
                wait_on(lo_in.at[b, i], lo_r.at[b, i])

    for b, (nf, ns) in enumerate(((nfx, nsx), (nfy, nsy))):
        g = jnp.sum(lo_in[b].astype(F32), axis=0)
        first = 0.8 * m_loc[b] + 0.2 * g
        second = 0.9 * m_loc[2 + b] + 0.1 * g * g
        nf[...] = first
        ns[...] = second
        d_out[b] = (first / jnp.sqrt(second)).astype(BF16)

    def far_sent():
        @pl.loop(0, NZ)
        def _(i):
            for b in range(2):
                @pl.when((i != z) | (b != c))
                def _():
                    wait_on(lo_out.at[0], far_s.at[i, b])

    far_sent()

    row = 2 * z + c

    @pl.loop(0, NZ)
    def _(i):
        k = lax.rem(i, 2) * (8 + (i + 1) // 2) + (1 - lax.rem(i, 2)) * (8 - i // 2)
        zt = lax.rem(z + k, NZ)
        for ct in range(2):
            @pl.when((k > 0) & (k < NZ))
            def _():
                send(d_out.at[ct], d_all.at[row], far_s.at[zt, ct], d_r.at[row], (zt, ct, y, x))

    d_all[row] = d_out[c]
    send(d_out.at[other], d_all.at[row], far_s.at[z, other], d_r.at[row], partner)
    ring(7)
    ring(8)
    wait_on(w_all.at[12], wr_r.at[0, 7])
    wait_on(w_all.at[11], wr_r.at[1, 6])
    send(w_all, w_oth, pr_s.at[3], pr_r.at[3], partner)

    @pl.loop(0, 32)
    def _(i):
        @pl.when(i != row)
        def _():
            wait_on(d_all.at[i], d_r.at[i])

    d = d_all[...].reshape(512, 128)
    squares = jnp.zeros((8, 128), F32)
    for t in range(4):
        u = jnp.dot(f_all[4 * t : 4 * t + 4].reshape(512, 512), d, preferred_element_type=F32)
        squares = squares + jnp.sum((u * u).reshape(64, 8, 128), axis=0)
        u_f[4 * t : 4 * t + 4] = u.reshape(4, 128, 128)
        u_b[4 * t : 4 * t + 4] = u.astype(BF16).reshape(4, 128, 128)
    squares = jnp.sum(squares, axis=0, keepdims=True)
    s_out[0] = squares
    s_all[place] = squares
    far_sent()

    @pl.loop(1, 32)
    def _(k):
        q = lax.rem(place + k, 32)
        send(s_out.at[0], s_all.at[place], far_s.at[q // 2, lax.rem(q, 2)], s_r.at[place], at_place(q))

    send(u_f.at[4, theirs, :], u_of, pr_s.at[4], pr_r.at[4], partner)
    send(u_b, u_ob, pr_s.at[5], pr_r.at[5], partner)

    @pl.loop(0, 32)
    def _(i):
        @pl.when(i != place)
        def _():
            wait_on(s_all.at[i], s_r.at[i])

    wait_on(u_of, pr_r.at[4])
    wait_on(u_ob, pr_r.at[5])
    wait_on(w_oth, pr_r.at[3])
    total = jnp.sum(jnp.sum(s_all[...], axis=0), axis=1, keepdims=True)
    scale = jnp.minimum(1.0, 0.25 * (2.0 * D * RW) ** 0.5 / jnp.sqrt(total))

    def finish(br, u_rows, st, nw, cp, wb, ub):
        step = scale * u_rows
        st[...] = step
        nw[...] = w_loc[br] - 0.02 * step

        @pl.loop(0, NZ)
        def _(i):
            at = pl.multiple_of(128 * lax.rem(z + i + (NZ - 4), NZ), 128)
            cp[pl.ds(at, 128), :] = (wb[i].astype(F32) - 0.02 * (scale * ub[i].astype(F32))).astype(BF16)

    @pl.when(c == 0)
    def _():
        finish(0, u_f[4, :64], stx, nwx, cpx, w_all, u_b)
        finish(1, u_of[...], sty, nwy, cpy, w_oth, u_ob)

    @pl.when(c == 1)
    def _():
        finish(1, u_f[4, 64:], sty, nwy, cpy, w_all, u_b)
        finish(0, u_of[...], stx, nwx, cpx, w_oth, u_ob)

    for br, a in enumerate((y, x)):
        @pl.when(c == a // 2)
        def _():
            for n in range(8):
                wait_on(slab(0), za_s.at[br, n])
    for m in range(4):
        wait_on(slab(0), zb_s.at[0, m])
    for m in range(3):
        wait_on(slab(0), zb_s.at[1, m])
    for g, (lo, n) in enumerate(groups):
        h = (n + 1) // 2
        for ph, (part, me) in enumerate(((part1, rb), (part2, ra))):
            for i, nn in enumerate((n, n, h, n - h)):
                wait_on(part(lo, nn, me), ip_s.at[g, ph, i])
    for i, r in enumerate((w_tmp, f_loc.at[0], g_in, w_oth, u_of, u_ob)):
        wait_on(r, pr_s.at[i])
    for s in range(8):
        wait_on(w_all.at[0], wr_s.at[0, s])
    for s in range(7):
        wait_on(w_all.at[0], wr_s.at[1, s])

    @pl.loop(1, 32)
    def _(k):
        q = lax.rem(place + k, 32)
        wait_on(s_out.at[0], far_s.at[q // 2, lax.rem(q, 2)])


def on_device(*args):
    out = lambda s, t: jax.ShapeDtypeStruct(s, t)
    dma = pltpu.SemaphoreType.DMA
    return pl.pallas_call(
        body,
        out_shape=[out((64, 128), F32)] * 4 + [out((16, 128), F32)] * 4 + [out((D, 128), BF16)] * 2,
        in_specs=[pl.BlockSpec(memory_space=pltpu.HBM)] * 11,
        out_specs=[pl.BlockSpec(memory_space=pltpu.VMEM)] * 10,
        scratch_shapes=[
            pltpu.VMEM((1024, D), BF16),
            pltpu.VMEM((1024, 256), BF16),
            pltpu.VMEM((2, 64, 512), BF16),
            pltpu.VMEM((2, 64, 128), F32),
            pltpu.VMEM((4, 16, 128), F32),
            pltpu.VMEM((NZ, 128, 512), BF16),
            pltpu.VMEM((2, 128, D), F32),
            pltpu.VMEM((128, D), F32),
            pltpu.VMEM((256, D), BF16),
            pltpu.VMEM((32, 16, 128), BF16),
            pltpu.VMEM((2, NZ, 16, 128), BF16),
            pltpu.VMEM((2, 16, 128), BF16),
            pltpu.VMEM((32, 16, 128), BF16),
            pltpu.VMEM((NZ, 128, 128), F32),
            pltpu.VMEM((NZ, 128, 128), BF16),
            pltpu.VMEM((NZ, 128, 128), BF16),
            pltpu.VMEM((64, 128), F32),
            pltpu.VMEM((NZ, 128, 128), BF16),
            pltpu.VMEM((64, 128), BF16),
            pltpu.VMEM((NZ, 128, 128), BF16),
            pltpu.VMEM((1, 1, 128), F32),
            pltpu.VMEM((32, 1, 128), F32),
            dma((11,)),
            dma((2, 8)),
            dma((NZ,)),
            dma((2, 4)),
            dma((3, 2, 4)),
            dma((3, 2, 4)),
            dma((6,)),
            dma((6,)),
            dma((2, 8)),
            dma((2, 8)),
            dma((NZ, 2)),
            dma((2, NZ)),
            dma((32,)),
            dma((32,)),
        ],
        compiler_params=pltpu.CompilerParams(
            collective_id=0, has_side_effects=True, vmem_limit_bytes=48 * 1024 * 1024
        ),
        name="update",
    )(*args)


def solution(mesh):
    split = Mesh(mesh.devices.reshape(NZ, 2, 4, 4), ("z", "c", "y", "x"))
    both = P(FS, TP)
    rows = P(FS, None)
    in_specs = (rows, both, both, both, both, rows, rows, both, both, both, both)
    out_specs = (both,) * 8 + (P(None, TP),) * 2
    return jax.shard_map(on_device, mesh=split, in_specs=in_specs, out_specs=out_specs, check_vma=False)
```
